32 devices in a mesh: fs: 16 (over z, y, core), tp: 2 (over x).
Axes of the slice: x: 2, y: 2, z: 4, core: 2. Of those that a mesh axis runs over, the one named last changes fastest.
Arguments:
- tokens: bfloat16 [8192, 2048], P('fs', 'tp'), may hold values from -6 to 6
- norm_gain: float32 [2048], P('fs'), may hold values from 0.1 to 1.9
- up_trained: float32 [2048, 4096], P('fs', 'tp'), may hold values from -0.125 to 0.125
- down_trained: float32 [4096, 2048], P('fs', 'tp'), may hold values from -0.09375 to 0.09375
Outputs:
- up_serving: bfloat16 [2048, 4096], P(None, 'tp')
- down_serving: bfloat16 [4096, 2048], P('tp')
- mixed: bfloat16 [8192, 2048], P('fs', 'tp')
The draws below stay inside these ranges and needn't reach their ends.
All inputs are finite; a program needn't handle non-finite values.
Results may differ from the reference program's by a relative error of at most 0.013.
Values may be sent and summed in bfloat16 or wider, within the bound.
No kernel may reach another device: no remote copies, remote signals or barrier semaphores. Data moves between devices by JAX's collectives and lax.ppermute only.
A program may use at most 128 MiB of HBM per device.

```python
import jax
import jax.numpy as jnp
from jax import lax

D = 2048
FF = 4096
TOKENS = 8192
N_TP = 2


def shard_levels(rng, dims, shards, least, largest):
    def one(axis_at, parts):
        steps = jax.random.uniform(jax.random.fold_in(jax.random.fold_in(rng, 6), axis_at), (parts,), jnp.float32, least / len(shards), largest / len(shards))
        return jnp.repeat(jnp.exp(steps), dims[axis_at] // parts).reshape((-1,) + (1,) * (len(dims) - axis_at - 1))

    loudness = one(*shards[0])
    for cut in shards[1:]:
        loudness = loudness * one(*cut)
    return loudness


def centred(own_key, dims, width, limit, cuts=(), dtype=jnp.bfloat16):
    loudness = shard_levels(own_key, dims, cuts, -0.22, 0.18) if cuts else 1.0
    array = jax.random.normal(own_key, dims, jnp.float32) * width * loudness
    return jnp.minimum(jnp.maximum(array, -limit), limit).astype(dtype)


def setup_inputs(seed: int = 0) -> dict:
    keys = jax.random.split(jax.random.key(seed), 5)
    tokens = centred(keys[0], (TOKENS, D), 1.0, 6.0, ((0, 16), (1, 2)))
    norm_gain = jnp.clip(1.0 + 0.18 * jax.random.normal(keys[1], (D,), jnp.float32), 0.1, 1.9)
    up_trained = centred(keys[2], (D, FF), D ** -0.5, 0.125, ((0, 16), (1, 2)), jnp.float32)
    down_trained = centred(keys[3], (FF, D), FF ** -0.5, 0.09375, ((0, 16), (1, 2)), jnp.float32)
    return {"tokens": tokens, "norm_gain": norm_gain, "up_trained": up_trained, "down_trained": down_trained}


def reference(tokens, norm_gain, up_trained, down_trained):
    up_serving = (norm_gain[:, None] * up_trained).astype(jnp.bfloat16)
    down_serving = down_trained.astype(jnp.bfloat16)
    widened = tokens.astype(jnp.float32)
    scale = lax.rsqrt(lax.optimization_barrier(jnp.mean(widened * widened, axis=-1, keepdims=True)) + 1e-06)
    normed = (widened * scale).astype(jnp.bfloat16)
    preact = jnp.dot(normed, up_serving, preferred_element_type=jnp.float32)
    hidden = jnp.square(jnp.maximum(preact, 0.0)).astype(jnp.bfloat16)
    block = FF // N_TP
    mixed = jnp.zeros((tokens.shape[0], D), jnp.float32)
    for index in range(N_TP):
        part = jnp.dot(hidden[:, index * block:(index + 1) * block], down_serving[index * block:(index + 1) * block], preferred_element_type=jnp.float32)
        rounded = lax.optimization_barrier(part.astype(jnp.bfloat16))
        mixed = mixed + rounded.astype(jnp.float32)
    return (up_serving, down_serving, mixed.astype(jnp.bfloat16))
```

```python
import jax
import jax.numpy as jnp
from jax import lax
from jax.sharding import PartitionSpec as P


def general(tokens, norm_gain, up_trained, down_trained):
    up_piece = (norm_gain[:, None] * up_trained).astype(jnp.bfloat16)
    up_serving = lax.all_gather(up_piece, "fs", axis=0, tiled=True)
    down_piece = down_trained.astype(jnp.bfloat16)
    group_count = lax.axis_size("fs")
    pair_count = lax.axis_size("tp")
    sliver = down_piece.shape[1] // group_count
    flipped = down_piece.T
    narrow = lax.all_to_all(flipped, "fs", split_axis=0, concat_axis=1, tiled=True)
    regrouped = lax.all_to_all(narrow, "tp", split_axis=1, concat_axis=0, tiled=True)
    spread = lax.all_gather(regrouped, "fs", axis=0, tiled=True)
    block_width = spread.shape[1]
    ordered = spread.reshape(group_count, pair_count, sliver, block_width).transpose(1, 0, 2, 3)
    down_serving = ordered.reshape(pair_count * group_count * sliver, block_width).T
    features = lax.all_gather(tokens, "tp", axis=1, tiled=True)
    normed = normalise(features)
    preact = jnp.dot(normed, up_serving, preferred_element_type=jnp.float32)
    hidden = jnp.square(jnp.maximum(preact, 0.0)).astype(jnp.bfloat16)
    partial_out = jnp.dot(hidden, down_serving, preferred_element_type=jnp.float32)
    summed = lax.psum_scatter(
        partial_out.astype(jnp.bfloat16), "tp", scatter_dimension=1, tiled=True
    )
    return (up_serving, down_serving, summed)


def normalise(features):
    widened = features.astype(jnp.float32)
    scale = lax.rsqrt(jnp.mean(widened * widened, axis=-1, keepdims=True) + 1e-06)
    return (widened * scale).astype(jnp.bfloat16)


Z, Y, C, T = 4, 2, 2, 2


def move(value, target):
    pairs = []
    for z in range(Z):
        for y in range(Y):
            for c in range(C):
                for t in range(T):
                    to = target(z, y, c, t)
                    if to is None:
                        continue
                    z2, y2, c2, t2 = to
                    pairs.append((((z * Y + y) * C + c) * T + t, ((z2 * Y + y2) * C + c2) * T + t2))
    return lax.ppermute(value, ("fs", "tp"), pairs)


def line(value, low, high, step):
    return move(value, lambda z, y, c, t: (z + step, y, c, t) if low <= z <= high else None)


def mirrored(value, hops):
    def target(z, y, c, t):
        m = z if t == 0 else Z - 1 - z
        if m not in hops:
            return None
        to = hops[m]
        return (to if t == 0 else Z - 1 - to, y, c, t)
    return move(value, target)


def across_y(value, keep=range(Z)):
    return move(value, lambda z, y, c, t: (z, 1 - y, c, t) if z in keep else None)


def across_core(value, keep=range(Z)):
    return move(value, lambda z, y, c, t: (z, y, 1 - c, t) if z in keep else None)


def across_tp(value):
    return move(value, lambda z, y, c, t: (z, y, c, 1 - t))


def put(buffer, piece, slot, y, c):
    return lax.dynamic_update_slice(buffer, piece[None, None, None], (slot, y, c, 0, 0))


def lined(tokens, norm_gain, up_trained, down_trained):
    i = lax.axis_index("fs")
    t = lax.axis_index("tp")
    c = i % C
    y = (i // C) % Y
    z = i // (C * Y)
    m = jnp.where(t == 0, z, Z - 1 - z)

    down_piece = down_trained.astype(jnp.bfloat16)
    crossed = move(
        down_piece, lambda z, y, c, t: (z, y, c, 1 - t) if z // (Z // T) != t else None
    )
    other_tokens = across_tp(tokens)

    up_piece = (norm_gain[:, None] * up_trained).astype(jnp.bfloat16)
    right1 = line(up_piece, 0, 2, 1)
    left1 = line(up_piece, 1, 3, -1)
    right2 = line(right1, 1, 2, 1)
    left2 = line(left1, 1, 2, -1)
    right3 = line(right2, 2, 2, 1)
    left3 = line(left2, 1, 1, -1)
    own_y = across_y(up_piece)
    rows, cols = up_piece.shape
    up_buffer = jnp.zeros((Z, Y, C, rows, cols), jnp.bfloat16)
    received = (
        (right1, (1, 2, 3), z >= 1, z - 1),
        (left1, (0, 1, 2), z <= 2, z + 1),
        (jnp.where(z >= 2, right2, left2), (0, 1, 2, 3), None, (z + 2) % Z),
        (jnp.where(z >= 2, right3, left3), (0, 3), (z == 0) | (z == 3), Z - 1 - z),
    )
    own = {(0, 0): up_piece, (1, 0): own_y, (0, 1): across_core(up_piece), (1, 1): across_core(own_y)}
    for piece, keep, valid, source in received:
        piece_y = across_y(piece, keep)
        variants = {
            (0, 0): piece,
            (1, 0): piece_y,
            (0, 1): across_core(piece, keep),
            (1, 1): across_core(piece_y, keep),
        }
        for (dy, dc), value in variants.items():
            slot = source
            if valid is not None:
                value = jnp.where(valid, value, own[dy, dc])
                slot = jnp.where(valid, source, z)
            up_buffer = put(up_buffer, value, slot, (y + dy) % Y, (c + dc) % C)
    up_serving = up_buffer.reshape(Z * Y * C * rows, cols)

    rows, cols = down_piece.shape
    first = jnp.where(m == 0, 0, 1)
    second = 1 - first
    first_slot = jnp.where(t == 0, first, 1 - first)
    second_slot = jnp.where(t == 0, second, 1 - second)

    def half(source):
        swapped = mirrored(source, {0: 1, 1: 0})
        near2 = mirrored(source, {1: 2})
        far2 = mirrored(swapped, {1: 2})
        near3 = mirrored(near2, {2: 3})
        far3 = mirrored(far2, {2: 3})
        near = jnp.where(m <= 1, source, jnp.where(m == 2, near2, near3))
        far = jnp.where(m <= 1, swapped, jnp.where(m == 2, far2, far3))
        buffer = jnp.zeros((Z // T, Y, C, rows, cols), jnp.bfloat16)
        for piece, slot in ((near, first_slot), (far, second_slot)):
            piece_y = across_y(piece)
            buffer = put(buffer, piece, slot, y, c)
            buffer = put(buffer, piece_y, slot, 1 - y, c)
            buffer = put(buffer, across_core(piece), slot, y, 1 - c)
            buffer = put(buffer, across_core(piece_y), slot, 1 - y, 1 - c)
        return buffer.reshape(Z // T * Y * C * rows, cols)

    given = half(crossed)
    kept = half(down_piece)
    down_serving = jnp.where(
        t == 0,
        jnp.concatenate([kept, given], axis=1),
        jnp.concatenate([given, kept], axis=1),
    )

    features = jnp.where(
        t == 0,
        jnp.concatenate([tokens, other_tokens], axis=1),
        jnp.concatenate([other_tokens, tokens], axis=1),
    )
    normed = normalise(features)
    preact = jnp.dot(normed, up_serving, preferred_element_type=jnp.float32)
    hidden = jnp.square(jnp.maximum(preact, 0.0)).astype(jnp.bfloat16)
    sent = jnp.dot(hidden, given, preferred_element_type=jnp.float32).astype(jnp.bfloat16)
    arrived = across_tp(sent)
    stays = jnp.dot(hidden, kept, preferred_element_type=jnp.float32).astype(jnp.bfloat16)
    mixed = (stays.astype(jnp.float32) + arrived.astype(jnp.float32)).astype(jnp.bfloat16)
    return (up_serving, down_serving, mixed)


def solution(mesh):
    placed = (P("fs", "tp"), P("fs"), P("fs", "tp"), P("fs", "tp"))
    fits = mesh.shape["fs"] == Z * Y * C and mesh.shape["tp"] == T
    return jax.shard_map(
        lined if fits else general,
        mesh=mesh,
        in_specs=placed,
        out_specs=(P(None, "tp"), P("tp", None), P("fs", "tp")),
        check_vma=False,
    )
```
